32 devices in a mesh: fs: 16 (over z, y, x), tp: 2 (over core).
Axes of the slice: x: 2, y: 2, z: 4, core: 2. Of those that a mesh axis runs over, the one named last changes fastest.
Arguments:
- tokens: bfloat16 [6144, 2048], P('fs', 'tp'), may hold values from -8 to 8
- w_value: bfloat16 [2048, 1024], P('fs', 'tp'), may hold values from -0.125 to 0.125
- w_gate: bfloat16 [2048, 1024], P('fs', 'tp'), may hold values from -0.125 to 0.125
- conv_kernel: bfloat16 [31, 1024], replicated, may hold values from -1 to 1
- conv_gain: float32 [1024], replicated, may hold values from 0.1 to 1.9
- w_mix_out: bfloat16 [1024, 2048], P('fs', 'tp'), may hold values from -0.1875 to 0.1875
- mix_gain: float32 [2048], replicated, may hold values from 0.1 to 1.9
- w_up: bfloat16 [2048, 8192], P('fs', 'tp'), may hold values from -0.125 to 0.125
- w_down: bfloat16 [8192, 2048], P('tp', 'fs'), may hold values from -0.0625 to 0.0625
- out_gain: float32 [2048], replicated, may hold values from 0.1 to 1.9
Outputs:
- result: bfloat16 [6144, 2048], P('fs', 'tp')
The draws below stay inside these ranges and needn't reach their ends.
All inputs are finite; a program needn't handle non-finite values.
Results may differ from the reference program's by a relative error of at most 0.013.
Values may be sent and summed in bfloat16 or wider, within the bound.
A program may use at most 128 MiB of HBM per device.

```python
import math
import jax
import jax.numpy as jnp
from jax import lax

WIDTH = 2048
CHANNELS = 1024
UNITS = 8192
KERNEL = 31
LENGTH = 128
TOK_DEV = 384
TOKENS = 6144
N_FS = 16
N_TP = 2


def draw_tokens(key, part):
    scale_key, value_key, shift_key = jax.random.split(jax.random.fold_in(key, 11), 3)
    block_scales = jnp.exp(jax.random.uniform(scale_key, (8,), jnp.float32, math.log(0.3), math.log(3.0)))
    column_scales = jnp.repeat(block_scales, WIDTH // 8)
    raw = jax.random.normal(value_key, (TOKENS, WIDTH), jnp.float32)
    return jnp.clip(raw * column_scales, -8.0, 8.0).astype(jnp.bfloat16)


def block_levels(key, dims, pieces, low, top_value):
    gain, own = 1.0, jax.random.fold_in(key, 6)
    for axis_at, blocks in pieces:
        steps = jnp.exp(jax.random.uniform(jax.random.fold_in(own, axis_at), (blocks,), jnp.float32, low / len(pieces), top_value / len(pieces)))
        gain = gain * jnp.repeat(steps, dims[axis_at] // blocks).reshape([-1 if axis == axis_at else 1 for axis in range(len(dims))])
    return gain


def bell_draw(stream_key, dims, deviation, bound, pieces=(), held_as=jnp.bfloat16):
    result = deviation * jax.random.normal(stream_key, dims, jnp.float32)
    if pieces:
        result = result * block_levels(stream_key, dims, pieces, -0.22, 0.18)
    return jnp.clip(result, -bound, bound).astype(held_as)


def setup_inputs(seed: int = 0) -> dict:
    streams_of = jax.random.split(jax.random.key(seed), 11)
    tokens = draw_tokens(jax.random.fold_in(streams_of[10], 71), 0)
    w_value = bell_draw(streams_of[1], (WIDTH, CHANNELS), WIDTH ** -0.5, 0.125, ((0, 16), (1, 2)))
    w_gate = bell_draw(streams_of[2], (WIDTH, CHANNELS), WIDTH ** -0.5, 0.125, ((0, 16), (1, 2)))
    conv_kernel = bell_draw(streams_of[3], (KERNEL, CHANNELS), KERNEL ** -0.5, 1.0)
    conv_gain = jnp.clip(1.0 + 0.18 * jax.random.normal(streams_of[4], (CHANNELS,), jnp.float32), 0.1, 1.9)
    w_mix_out = bell_draw(streams_of[5], (CHANNELS, WIDTH), CHANNELS ** -0.5, 0.1875, ((0, 16), (1, 2)))
    mix_gain = jnp.clip(1.0 + 0.18 * jax.random.normal(streams_of[6], (WIDTH,), jnp.float32), 0.1, 1.9)
    w_up = bell_draw(streams_of[7], (WIDTH, UNITS), WIDTH ** -0.5, 0.125, ((0, 16), (1, 2)))
    w_down = bell_draw(streams_of[8], (UNITS, WIDTH), UNITS ** -0.5, 0.0625, ((0, 2), (1, 16)))
    out_gain = jnp.clip(1.0 + 0.18 * jax.random.normal(streams_of[9], (WIDTH,), jnp.float32), 0.1, 1.9)
    return {"tokens": tokens, "w_value": w_value, "w_gate": w_gate, "conv_kernel": conv_kernel, "conv_gain": conv_gain, "w_mix_out": w_mix_out, "mix_gain": mix_gain, "w_up": w_up, "w_down": w_down, "out_gain": out_gain}


norm_eps = 1e-05
residual_scale = 2.0 ** 0.5

def causal_filter(gated, kernel):
    sequences = gated.shape[0] // LENGTH
    frames = gated.astype(jnp.float32).reshape(sequences, LENGTH, gated.shape[1])
    padded = jnp.pad(frames, ((0, 0), (KERNEL - 1, 0), (0, 0)))
    accumulated = jnp.zeros(frames.shape, jnp.float32)
    for offset in range(KERNEL):
        accumulated = accumulated + kernel[offset].astype(jnp.float32) * padded[:, offset:offset + LENGTH]
    return accumulated.reshape(gated.shape[0], gated.shape[1])

def normalize(values, total_sum, total_sq, entries, gain_vector):
    average = total_sum / entries
    spread = jnp.maximum(total_sq / entries - average * average, 0.0)
    return (values - average[:, None]) * lax.rsqrt(spread[:, None] + norm_eps) * gain_vector.astype(jnp.float32)

def reference(tokens, w_value, w_gate, conv_kernel, conv_gain, w_mix_out, mix_gain, w_up, w_down, out_gain):

    def one_block(frames):
        values_proj = jnp.dot(frames, w_value, preferred_element_type=jnp.float32)
        gate_proj = jnp.dot(frames, w_gate, preferred_element_type=jnp.float32)
        gated = (values_proj * jax.nn.sigmoid(gate_proj)).astype(jnp.bfloat16)
        filtered = causal_filter(gated, conv_kernel)
        normed = normalize(filtered, lax.optimization_barrier(jnp.sum(filtered, 1)), lax.optimization_barrier(jnp.sum(filtered * filtered, 1)), CHANNELS, conv_gain)
        activated = jax.nn.silu(normed).astype(jnp.bfloat16)
        mixed = jnp.dot(activated, w_mix_out, preferred_element_type=jnp.float32)
        combined = residual_scale * frames.astype(jnp.float32) + mixed
        middle = normalize(combined, lax.optimization_barrier(jnp.sum(combined, 1)), lax.optimization_barrier(jnp.sum(combined * combined, 1)), WIDTH, mix_gain).astype(jnp.bfloat16)
        up_proj = jnp.dot(middle, w_up, preferred_element_type=jnp.float32)
        hidden = jnp.square(jax.nn.relu(up_proj)).astype(jnp.bfloat16)
        share_size = UNITS // N_TP
        down_sum = jnp.zeros((frames.shape[0], WIDTH), jnp.float32)
        for block_index in range(N_TP):
            lower = block_index * share_size
            piece_sum = jnp.dot(hidden[:, lower:lower + share_size], w_down[lower:lower + share_size], preferred_element_type=jnp.float32).astype(jnp.bfloat16)
            piece_sum = lax.optimization_barrier(piece_sum)
            down_sum = down_sum + piece_sum.astype(jnp.float32)
        final = residual_scale * middle.astype(jnp.float32) + down_sum
        return normalize(final, lax.optimization_barrier(jnp.sum(final, 1)), lax.optimization_barrier(jnp.sum(final * final, 1)), WIDTH, out_gain).astype(jnp.bfloat16)
    blocks = tokens.reshape(N_FS, TOK_DEV, WIDTH)
    return lax.map(one_block, blocks).reshape(TOKENS, WIDTH)
```

```python
import functools
import jax
import jax.numpy as jnp
from jax import lax
from jax.sharding import PartitionSpec as P

KERNEL = 31
LENGTH = 128


norm_eps = 1e-05
residual_scale = 2.0**0.5


def causal_filter(gated, kernel):
    sequences = gated.shape[0] // LENGTH
    frames = gated.astype(jnp.float32).reshape(sequences, LENGTH, gated.shape[1])
    padded = jnp.pad(frames, ((0, 0), (KERNEL - 1, 0), (0, 0)))
    accumulated = jnp.zeros(frames.shape, jnp.float32)
    for offset in range(KERNEL):
        accumulated = (
            accumulated + kernel[offset].astype(jnp.float32) * padded[:, offset : offset + LENGTH]
        )
    return accumulated.reshape(gated.shape[0], gated.shape[1])


def normalize(values, total_sum, total_sq, entries, gain_vector):
    average = total_sum / entries
    spread = jnp.maximum(total_sq / entries - average * average, 0.0)
    return (values - average[:, None]) * lax.rsqrt(spread[:, None] + norm_eps) * gain_vector


PLANE = 4


def per_device(
    n_fs,
    n_tp,
    tokens,
    w_value,
    w_gate,
    conv_kernel,
    conv_gain,
    w_mix_out,
    mix_gain,
    w_up,
    w_down,
    out_gain,
):
    lines = n_fs // PLANE
    fs_rank = lax.axis_index("fs")
    line, place = fs_rank // PLANE, fs_rank % PLANE
    tp_rank = lax.axis_index("tp")
    frames, width_part = tokens.shape
    channel_part = w_value.shape[1]
    width, channels = width_part * n_tp, channel_part * n_tp

    def swap(array, mask):
        pairs = [(f, (f // PLANE) * PLANE + ((f % PLANE) ^ mask)) for f in range(n_fs)]
        return lax.ppermute(array, "fs", pairs)

    def shift(array, step, upward):
        if upward:
            moves = [(a, a + 1) for a in range(step - 1, lines - 1)]
        else:
            moves = [(a, a - 1) for a in range(1, lines - step + 1)]
        pairs = [(a * PLANE + q, b * PLANE + q) for a, b in moves for q in range(PLANE)]
        return lax.ppermute(array, "fs", pairs)

    def put(buffer, block, index):
        return lax.dynamic_update_slice_in_dim(buffer, block[None], index, 0)

    def line_gather(block):
        ups, downs = [block], [block]
        for step in range(1, lines):
            ups.append(shift(ups[-1], step, True))
            downs.append(shift(downs[-1], step, False))
        out = put(jnp.zeros((lines,) + block.shape, block.dtype), block, line)
        for step in range(1, lines):
            piece = jnp.where(line >= step, ups[step], downs[lines - step])
            out = put(out, piece, (line - step) % lines)
        return out

    def plane_gather(block):
        across, along = swap(block, 1), swap(block, 2)
        half = block.shape[0] // 2
        far = jnp.concatenate([swap(along[:half], 1), swap(across[half:], 2)], 0)
        out = jnp.zeros((PLANE,) + block.shape, block.dtype)
        for mask, piece in enumerate((block, across, along, far)):
            out = put(out, piece, place ^ mask)
        return out

    def tp_gather(block):
        out = put(jnp.zeros((n_tp,) + block.shape, block.dtype), block, tp_rank)
        for step in range(1, n_tp):
            piece = lax.ppermute(block, "tp", [(i, (i + step) % n_tp) for i in range(n_tp)])
            out = put(out, piece, (tp_rank - step) % n_tp)
        return out

    def plane_exchange(pieces):
        own = lax.dynamic_index_in_dim(pieces, place, 0, False)
        out = put(jnp.zeros_like(pieces), own, place)
        for mask in range(1, PLANE):
            sent = lax.dynamic_index_in_dim(pieces, place ^ mask, 0, False)
            out = put(out, swap(sent, mask), place ^ mask)
        return out

    pair_block = jnp.concatenate([w_value, w_gate], 1)
    pair_whole = plane_gather(line_gather(pair_block))
    pair_whole = pair_whole.reshape(width, 2 * channel_part)
    rows = w_value.shape[0]
    mix_rows = w_mix_out.shape[0]
    mix_whole = plane_gather(line_gather(w_mix_out))
    mix_whole = jnp.swapaxes(mix_whole, 0, 1).reshape(channels, width_part)

    units = w_up.shape[1]
    quarter = units // PLANE
    up_pieces = jnp.swapaxes(w_up.reshape(rows, PLANE, quarter), 0, 1)
    up_chunk = plane_exchange(up_pieces).reshape(PLANE * rows, quarter)
    up_whole = line_gather(up_chunk).reshape(width, quarter)
    cols = w_down.shape[1]
    down_pieces = w_down.reshape(PLANE, quarter, cols)
    down_chunk = jnp.swapaxes(plane_exchange(down_pieces), 0, 1).reshape(quarter, PLANE * cols)
    down_whole = line_gather(down_chunk)

    features = jnp.swapaxes(tp_gather(tokens), 0, 1).reshape(frames, width)
    features = jnp.swapaxes(features.reshape(frames, lines, PLANE, rows), 1, 2)
    both = jnp.dot(
        features.reshape(frames, width), pair_whole, preferred_element_type=jnp.float32
    )
    values_proj, gate_proj = both[:, :channel_part], both[:, channel_part:]
    gated = (values_proj * jax.nn.sigmoid(gate_proj)).astype(jnp.bfloat16)
    kernel = lax.dynamic_slice_in_dim(conv_kernel, tp_rank * channel_part, channel_part, 1)
    filtered = causal_filter(gated, kernel)
    channel_sum, channel_sq = lax.psum(
        (jnp.sum(filtered, 1), jnp.sum(filtered * filtered, 1)), "tp"
    )
    channel_gain = lax.dynamic_slice_in_dim(conv_gain, tp_rank * channel_part, channel_part, 0)
    activated = jax.nn.silu(
        normalize(filtered, channel_sum, channel_sq, channels, channel_gain)
    ).astype(jnp.bfloat16)
    all_channels = jnp.swapaxes(tp_gather(activated), 0, 1).reshape(frames, channels)
    mixed = jnp.dot(all_channels, mix_whole, preferred_element_type=jnp.float32)
    combined = residual_scale * tokens.astype(jnp.float32) + mixed
    middle_sum, middle_sq = lax.psum((jnp.sum(combined, 1), jnp.sum(combined * combined, 1)), "tp")
    middle_gain = lax.dynamic_slice_in_dim(mix_gain, tp_rank * width_part, width_part, 0)
    middle = normalize(combined, middle_sum, middle_sq, width, middle_gain).astype(jnp.bfloat16)

    plane_part = plane_gather(middle).reshape(PLANE * frames, width_part)
    plane_whole = jnp.swapaxes(tp_gather(plane_part), 0, 1).reshape(PLANE * frames, width)
    up_proj = jnp.dot(plane_whole, up_whole, preferred_element_type=jnp.float32)
    hidden = jnp.square(jax.nn.relu(up_proj)).astype(jnp.bfloat16)
    terms = jnp.concatenate(
        [
            jnp.dot(hidden, down_whole[at], preferred_element_type=jnp.float32).astype(
                jnp.bfloat16
            )
            for at in range(lines)
        ],
        1,
    )
    part = lax.dynamic_slice_in_dim(terms, tp_rank * width_part, width_part, 1).astype(jnp.float32)
    for step in range(1, n_tp):
        target = (tp_rank + step) % n_tp
        sent = lax.dynamic_slice_in_dim(terms, target * width_part, width_part, 1)
        came = lax.ppermute(sent, "tp", [(i, (i + step) % n_tp) for i in range(n_tp)])
        part = part + came.astype(jnp.float32)
    part = part.reshape(PLANE, frames, width_part)
    down_sum = lax.dynamic_index_in_dim(part, place, 0, False)
    part = part.astype(jnp.bfloat16)
    for mask in range(1, PLANE):
        sent = lax.dynamic_index_in_dim(part, place ^ mask, 0, False)
        down_sum = down_sum + swap(sent, mask).astype(jnp.float32)
    final = residual_scale * middle.astype(jnp.float32) + down_sum
    final_sum, final_sq = lax.psum((jnp.sum(final, 1), jnp.sum(final * final, 1)), "tp")
    final_gain = lax.dynamic_slice_in_dim(out_gain, tp_rank * width_part, width_part, 0)
    return normalize(final, final_sum, final_sq, width, final_gain).astype(jnp.bfloat16)


def solution(mesh):
    in_specs = (
        P("fs", "tp"),
        P("fs", "tp"),
        P("fs", "tp"),
        P(),
        P(),
        P("fs", "tp"),
        P(),
        P("fs", "tp"),
        P("tp", "fs"),
        P(),
    )
    out_specs = P("fs", "tp")
    return jax.shard_map(
        functools.partial(per_device, mesh.shape["fs"], mesh.shape["tp"]),
        mesh=mesh, in_specs=in_specs, out_specs=out_specs, check_vma=False
    )
```

```python
import functools
import jax
import jax.numpy as jnp
from jax import lax
from jax.sharding import PartitionSpec as P


KERNEL = 31
LENGTH = 128


norm_eps = 1e-05
residual_scale = 2.0**0.5


def causal_filter(gated, kernel):
    sequences = gated.shape[0] // LENGTH
    frames = gated.astype(jnp.float32).reshape(sequences, LENGTH, gated.shape[1])
    padded = jnp.pad(frames, ((0, 0), (KERNEL - 1, 0), (0, 0)))
    accumulated = jnp.zeros(frames.shape, jnp.float32)
    for offset in range(KERNEL):
        accumulated = (
            accumulated + kernel[offset].astype(jnp.float32) * padded[:, offset : offset + LENGTH]
        )
    return accumulated.reshape(gated.shape[0], gated.shape[1])


def normalize(values, total_sum, total_sq, entries, gain_vector):
    average = total_sum / entries
    spread = jnp.maximum(total_sq / entries - average * average, 0.0)
    return (values - average[:, None]) * lax.rsqrt(spread[:, None] + norm_eps) * gain_vector


PLANE = 4


def layer(
    n_fs,
    n_tp,
    tokens,
    w_value,
    w_gate,
    conv_kernel,
    conv_gain,
    w_mix_out,
    mix_gain,
    w_up,
    w_down,
    out_gain,
):
    lines = n_fs // PLANE
    fs_rank = lax.axis_index("fs")
    line, place = fs_rank // PLANE, fs_rank % PLANE
    tp_rank = lax.axis_index("tp")
    frames, width_part = tokens.shape
    channel_part = w_value.shape[1]
    width, channels = width_part * n_tp, channel_part * n_tp

    def swap(array, mask):
        pairs = [(f, (f // PLANE) * PLANE + ((f % PLANE) ^ mask)) for f in range(n_fs)]
        return lax.ppermute(array, "fs", pairs)

    def shift(array, step, upward, first=0):
        if upward:
            moves = [(a, a + step) for a in range(first, lines - step)]
        else:
            moves = [(a, a - step) for a in range(step, lines - first)]
        pairs = [(a * PLANE + q, b * PLANE + q) for a, b in moves for q in range(PLANE)]
        return lax.ppermute(array, "fs", pairs)

    def put(buffer, block, index, axis=0):
        return lax.dynamic_update_slice_in_dim(buffer, jnp.expand_dims(block, axis), index, axis)

    def line_gather(block, direct):
        ups, downs = [block], [block]
        for step in range(1, lines):
            if step <= direct:
                ups.append(shift(block, step, True))
                downs.append(shift(block, step, False))
            else:
                ups.append(shift(ups[-1], 1, True, step - 1))
                downs.append(shift(downs[-1], 1, False, step - 1))
        out = put(jnp.zeros((lines,) + block.shape, block.dtype), block, line)
        for step in range(1, lines):
            piece = jnp.where(line >= step, ups[step], downs[lines - step])
            out = put(out, piece, (line - step) % lines)
        return out

    def plane_gather(block, axis):
        across, along = swap(block, 1), swap(block, 2)
        half = block.shape[0] // 2
        far = jnp.concatenate([swap(along[:half], 1), swap(across[half:], 2)], 0)
        shape = block.shape[:axis] + (PLANE,) + block.shape[axis:]
        out = jnp.zeros(shape, block.dtype)
        for mask, piece in enumerate((block, across, along, far)):
            out = put(out, piece, place ^ mask, axis)
        return out

    def tp_shift(block, step):
        return lax.ppermute(block, "tp", [(i, (i + step) % n_tp) for i in range(n_tp)])

    def tp_dot(block, weights):
        parts = weights.reshape((n_tp, -1) + weights.shape[1:])
        total = None
        for step in range(n_tp):
            piece = block if step == 0 else tp_shift(block, step)
            rows_at = lax.dynamic_index_in_dim(parts, (tp_rank - step) % n_tp, 0, False)
            term = jnp.dot(piece, rows_at, preferred_element_type=jnp.float32)
            total = term if total is None else total + term
        return total

    def plane_exchange(pieces):
        own = lax.dynamic_index_in_dim(pieces, place, 0, False)
        out = put(jnp.zeros_like(pieces), own, place)
        for mask in range(1, PLANE):
            sent = lax.dynamic_index_in_dim(pieces, place ^ mask, 0, False)
            came = swap(sent, mask)
            out = put(out, came, place ^ mask)
        return out

    pair_block = jnp.concatenate([w_value, w_gate], 1)
    pair_whole = plane_gather(line_gather(pair_block, lines), 1).reshape(width, 2 * channel_part)
    rows = w_value.shape[0]
    mix_whole = plane_gather(line_gather(w_mix_out, lines), 1).reshape(channels, width_part)

    units = w_up.shape[1]
    quarter = units // PLANE
    up_pieces = jnp.swapaxes(w_up.reshape(rows, PLANE, quarter), 0, 1)
    up_chunk = plane_exchange(up_pieces).reshape(PLANE * rows, quarter)
    up_whole = line_gather(up_chunk, 2).reshape(width, quarter)
    cols = w_down.shape[1]
    down_pieces = w_down.reshape(PLANE, quarter, cols)
    down_chunk = jnp.swapaxes(plane_exchange(down_pieces), 0, 1).reshape(quarter, PLANE * cols)
    down_whole = line_gather(down_chunk, 2)

    both = tp_dot(tokens, pair_whole)
    values_proj, gate_proj = both[:, :channel_part], both[:, channel_part:]
    gated = (values_proj * jax.nn.sigmoid(gate_proj)).astype(jnp.bfloat16)
    kernel = lax.dynamic_slice_in_dim(conv_kernel, tp_rank * channel_part, channel_part, 1)
    filtered = causal_filter(gated, kernel)
    channel_sum, channel_sq = lax.psum(
        (jnp.sum(filtered, 1), jnp.sum(filtered * filtered, 1)), "tp"
    )
    channel_gain = lax.dynamic_slice_in_dim(conv_gain, tp_rank * channel_part, channel_part, 0)
    activated = jax.nn.silu(
        normalize(filtered, channel_sum, channel_sq, channels, channel_gain)
    ).astype(jnp.bfloat16)
    mixed = tp_dot(activated, mix_whole)
    combined = residual_scale * tokens.astype(jnp.float32) + mixed
    middle_sum, middle_sq = lax.psum((jnp.sum(combined, 1), jnp.sum(combined * combined, 1)), "tp")
    middle_gain = lax.dynamic_slice_in_dim(mix_gain, tp_rank * width_part, width_part, 0)
    middle = normalize(combined, middle_sum, middle_sq, width, middle_gain).astype(jnp.bfloat16)

    plane_part = plane_gather(middle, 0).reshape(PLANE * frames, width_part)
    hidden = jnp.square(jax.nn.relu(tp_dot(plane_part, up_whole))).astype(jnp.bfloat16)

    per_core = lines // n_tp

    def product(core, at):
        weights = lax.dynamic_index_in_dim(down_whole, core * per_core + at, 0, False)
        return jnp.dot(hidden, weights, preferred_element_type=jnp.float32)

    came = []
    for step in range(1, n_tp):
        sent = [product((tp_rank + step) % n_tp, at) for at in range(per_core)]
        came.append([tp_shift(piece.astype(jnp.bfloat16), step) for piece in sent])
    chunks = []
    for at in range(per_core):
        chunk = product(tp_rank, at)
        for arrived in came:
            chunk = chunk + arrived[at].astype(jnp.float32)
        chunks.append(chunk.reshape(PLANE, frames, PLANE * cols))

    def of_place(part, mask):
        return lax.dynamic_index_in_dim(part, place ^ mask, 0, False)

    def plane_sum(part, mask_first, mask_second):
        sent = jnp.stack([of_place(part, mask_first), of_place(part, 3)]).astype(jnp.bfloat16)
        arrived = swap(sent, mask_first).astype(jnp.float32)
        onward = (of_place(part, mask_second) + arrived[1]).astype(jnp.bfloat16)
        return of_place(part, 0) + arrived[0] + swap(onward, mask_second).astype(jnp.float32)

    down_sum = jnp.concatenate(
        [
            plane_sum(chunk, 1, 2) if at % 2 == 0 else plane_sum(chunk, 2, 1)
            for at, chunk in enumerate(chunks)
        ],
        1,
    )
    final = residual_scale * middle.astype(jnp.float32) + down_sum
    final_sum, final_sq = lax.psum((jnp.sum(final, 1), jnp.sum(final * final, 1)), "tp")
    final_gain = lax.dynamic_slice_in_dim(out_gain, tp_rank * width_part, width_part, 0)
    return normalize(final, final_sum, final_sq, width, final_gain).astype(jnp.bfloat16)


def solution(mesh):
    in_specs = (
        P("fs", "tp"),
        P("fs", "tp"),
        P("fs", "tp"),
        P(),
        P(),
        P("fs", "tp"),
        P(),
        P("fs", "tp"),
        P("tp", "fs"),
        P(),
    )
    out_specs = P("fs", "tp")
    return jax.shard_map(
        functools.partial(layer, mesh.shape["fs"], mesh.shape["tp"]),
        mesh=mesh,
        in_specs=in_specs,
        out_specs=out_specs,
        check_vma=False,
    )
```

```python
import functools
import jax
import jax.numpy as jnp
from jax import lax
from jax.sharding import PartitionSpec as P


KERNEL = 31
LENGTH = 128


norm_eps = 1e-05
residual_scale = 2.0**0.5


def causal_filter(gated, kernel):
    sequences = gated.shape[0] // LENGTH
    frames = gated.astype(jnp.float32).reshape(sequences, LENGTH, gated.shape[1])
    padded = jnp.pad(frames, ((0, 0), (KERNEL - 1, 0), (0, 0)))
    accumulated = jnp.zeros(frames.shape, jnp.float32)
    for offset in range(KERNEL):
        accumulated = (
            accumulated + kernel[offset].astype(jnp.float32) * padded[:, offset : offset + LENGTH]
        )
    return accumulated.reshape(gated.shape[0], gated.shape[1])


def normalize(values, total_sum, total_sq, entries, gain_vector):
    average = total_sum / entries
    spread = jnp.maximum(total_sq / entries - average * average, 0.0)
    return (values - average[:, None]) * lax.rsqrt(spread[:, None] + norm_eps) * gain_vector


PLANE = 4


def layer(
    n_fs,
    n_tp,
    tokens,
    w_value,
    w_gate,
    conv_kernel,
    conv_gain,
    w_mix_out,
    mix_gain,
    w_up,
    w_down,
    out_gain,
):
    lines = n_fs // PLANE
    fs_rank = lax.axis_index("fs")
    line, place = fs_rank // PLANE, fs_rank % PLANE
    tp_rank = lax.axis_index("tp")
    frames, width_part = tokens.shape
    channel_part = w_value.shape[1]
    width, channels = width_part * n_tp, channel_part * n_tp

    def swap(array, mask):
        pairs = [(f, (f // PLANE) * PLANE + ((f % PLANE) ^ mask)) for f in range(n_fs)]
        return lax.ppermute(array, "fs", pairs)

    def cross(array, mask):
        pairs = [(f, ((f // PLANE) ^ mask) * PLANE + f % PLANE) for f in range(n_fs)]
        return lax.ppermute(array, "fs", pairs)

    def put(buffer, block, index, axis=0):
        return lax.dynamic_update_slice_in_dim(buffer, jnp.expand_dims(block, axis), index, axis)

    def line_gather(block):
        held = {0: block}
        mask = lines // 2
        while mask:
            for at, piece in list(held.items()):
                held[at ^ mask] = cross(piece, mask)
            mask //= 2
        out = jnp.zeros((lines,) + block.shape, block.dtype)
        for at, piece in held.items():
            out = put(out, piece, line ^ at)
        return out

    def plane_gather(block, axis):
        across, along = swap(block, 1), swap(block, 2)
        half = block.shape[0] // 2
        far = jnp.concatenate([swap(along[:half], 1), swap(across[half:], 2)], 0)
        shape = block.shape[:axis] + (PLANE,) + block.shape[axis:]
        out = jnp.zeros(shape, block.dtype)
        for mask, piece in enumerate((block, across, along, far)):
            out = put(out, piece, place ^ mask, axis)
        return out

    def tp_shift(block, step):
        return lax.ppermute(block, "tp", [(i, (i + step) % n_tp) for i in range(n_tp)])

    def tp_dot(block, weights):
        parts = weights.reshape((n_tp, -1) + weights.shape[1:])
        total = None
        for step in range(n_tp):
            piece = block if step == 0 else tp_shift(block, step)
            rows_at = lax.dynamic_index_in_dim(parts, (tp_rank - step) % n_tp, 0, False)
            term = jnp.dot(piece, rows_at, preferred_element_type=jnp.float32)
            total = term if total is None else total + term
        return total

    def plane_exchange(pieces):
        own = lax.dynamic_index_in_dim(pieces, place, 0, False)
        out = put(jnp.zeros_like(pieces), own, place)
        for mask in range(1, PLANE):
            sent = lax.dynamic_index_in_dim(pieces, place ^ mask, 0, False)
            came = swap(sent, mask)
            out = put(out, came, place ^ mask)
        return out

    pair_block = jnp.concatenate([w_value, w_gate], 1)
    pair_whole = plane_gather(line_gather(pair_block), 1).reshape(width, 2 * channel_part)
    rows = w_value.shape[0]
    mix_whole = plane_gather(line_gather(w_mix_out), 1).reshape(channels, width_part)

    units = w_up.shape[1]
    quarter = units // PLANE
    up_pieces = jnp.swapaxes(w_up.reshape(rows, PLANE, quarter), 0, 1)
    up_chunk = plane_exchange(up_pieces).reshape(PLANE * rows, quarter)
    up_whole = line_gather(up_chunk).reshape(width, quarter)
    cols = w_down.shape[1]
    down_pieces = w_down.reshape(PLANE, quarter, cols)
    down_chunk = jnp.swapaxes(plane_exchange(down_pieces), 0, 1).reshape(quarter, PLANE * cols)
    down_whole = line_gather(down_chunk)

    both = tp_dot(tokens, pair_whole)
    values_proj, gate_proj = both[:, :channel_part], both[:, channel_part:]
    gated = (values_proj * jax.nn.sigmoid(gate_proj)).astype(jnp.bfloat16)
    kernel = lax.dynamic_slice_in_dim(conv_kernel, tp_rank * channel_part, channel_part, 1)
    filtered = causal_filter(gated, kernel)
    channel_sum, channel_sq = lax.psum(
        (jnp.sum(filtered, 1), jnp.sum(filtered * filtered, 1)), "tp"
    )
    channel_gain = lax.dynamic_slice_in_dim(conv_gain, tp_rank * channel_part, channel_part, 0)
    activated = jax.nn.silu(
        normalize(filtered, channel_sum, channel_sq, channels, channel_gain)
    ).astype(jnp.bfloat16)
    mixed = tp_dot(activated, mix_whole)
    combined = residual_scale * tokens.astype(jnp.float32) + mixed
    middle_sum, middle_sq = lax.psum((jnp.sum(combined, 1), jnp.sum(combined * combined, 1)), "tp")
    middle_gain = lax.dynamic_slice_in_dim(mix_gain, tp_rank * width_part, width_part, 0)
    middle = normalize(combined, middle_sum, middle_sq, width, middle_gain).astype(jnp.bfloat16)

    plane_part = plane_gather(middle, 0).reshape(PLANE * frames, width_part)
    hidden = jnp.square(jax.nn.relu(tp_dot(plane_part, up_whole))).astype(jnp.bfloat16)

    per_core = lines // n_tp

    def product(core, at):
        weights = lax.dynamic_index_in_dim(down_whole, core * per_core + at, 0, False)
        return jnp.dot(hidden, weights, preferred_element_type=jnp.float32)

    came = []
    for step in range(1, n_tp):
        sent = [product((tp_rank + step) % n_tp, at) for at in range(per_core)]
        came.append([tp_shift(piece.astype(jnp.bfloat16), step) for piece in sent])
    chunks = []
    for at in range(per_core):
        chunk = product(tp_rank, at)
        for arrived in came:
            chunk = chunk + arrived[at].astype(jnp.float32)
        chunks.append(chunk.reshape(PLANE, frames, PLANE * cols))

    def of_place(part, mask):
        return lax.dynamic_index_in_dim(part, place ^ mask, 0, False)

    def plane_sum(part, mask_first, mask_second):
        sent = jnp.stack([of_place(part, mask_first), of_place(part, 3)]).astype(jnp.bfloat16)
        arrived = swap(sent, mask_first).astype(jnp.float32)
        onward = (of_place(part, mask_second) + arrived[1]).astype(jnp.bfloat16)
        return of_place(part, 0) + arrived[0] + swap(onward, mask_second).astype(jnp.float32)

    down_sum = jnp.concatenate(
        [
            plane_sum(chunk, 1, 2) if at % 2 == 0 else plane_sum(chunk, 2, 1)
            for at, chunk in enumerate(chunks)
        ],
        1,
    )
    final = residual_scale * middle.astype(jnp.float32) + down_sum
    final_sum, final_sq = lax.psum((jnp.sum(final, 1), jnp.sum(final * final, 1)), "tp")
    final_gain = lax.dynamic_slice_in_dim(out_gain, tp_rank * width_part, width_part, 0)
    return normalize(final, final_sum, final_sq, width, final_gain).astype(jnp.bfloat16)


def solution(mesh):
    in_specs = (
        P("fs", "tp"),
        P("fs", "tp"),
        P("fs", "tp"),
        P(),
        P(),
        P("fs", "tp"),
        P(),
        P("fs", "tp"),
        P("tp", "fs"),
        P(),
    )
    out_specs = P("fs", "tp")
    return jax.shard_map(
        functools.partial(layer, mesh.shape["fs"], mesh.shape["tp"]),
        mesh=mesh,
        in_specs=in_specs,
        out_specs=out_specs,
        check_vma=False,
    )
```
